512 devices in a mesh: sp: 32 (over z, x), tp: 16 (over y, core).
Axes of the slice: x: 4, y: 8, z: 8, core: 2. Of those that a mesh axis runs over, the one named last changes fastest.
Arguments:
- pool_input: bfloat16 [4096, 1024], P('sp', 'tp'), may hold values from -12 to 12
- doc_ids: int32 [4096], P('sp'), may hold values from 0 to 7, as said below
- residual: bfloat16 [4096, 2048], P('sp', 'tp'), may hold values from -30 to 30
- pool_gain: float32 [1024], P('tp'), may hold values from 0.1 to 1.9
- out_proj: bfloat16 [1024, 2048], P('tp'), may hold values from -0.25 to 0.25
- norm_gain: float32 [2048], P('tp'), may hold values from 0.1 to 1.9
- routes: int32 [4096, 2], P('sp'), may hold values from 0 to 31, all different within a row; in each aligned block of 128 rows (0 to 127, 128 to 255, ...) at most 16 rows name the same one
- route_weights: float32 [4096, 2], P('sp'), may hold values from 0.2 to 1.2
- expert_gate: bfloat16 [32, 2048, 4096], P('sp', None, 'tp'), may hold values from -0.125 to 0.125
- expert_up: bfloat16 [32, 2048, 4096], P('sp', None, 'tp'), may hold values from -0.125 to 0.125
- expert_down: bfloat16 [32, 4096, 2048], P('sp', 'tp'), may hold values from -0.125 to 0.125
- shared_gate: bfloat16 [2048, 1024], P(None, 'tp'), may hold values from -0.125 to 0.125
- shared_up: bfloat16 [2048, 1024], P(None, 'tp'), may hold values from -0.125 to 0.125
- shared_down: bfloat16 [1024, 2048], P('tp'), may hold values from -0.25 to 0.25
Outputs:
- layer_out: bfloat16 [4096, 2048], P('sp', 'tp')
The draws below stay inside these ranges and needn't reach their ends.
Inputs may be any that keep to these rules, and one draw needn't show every extreme that they name: `routes`: each row names 2 different experts. In each aligned block of 128 rows no expert is named by more than 16 rows; in some blocks one expert is named by exactly 16 rows. `doc_ids`: document numbers start at 0, never fall along the sequence and rise by one at each document's start.
All inputs are finite; a program needn't handle non-finite values.
Results may differ from the reference program's by a relative error of at most 0.015.
Values may be sent and summed in bfloat16 or wider, within the bound.
A program may use at most 64 MiB of HBM per device.

```python
import math
import jax
import jax.numpy as jnp
import numpy as np
from jax import lax

D = 2048
PW = 1024
FF_E = 4096
FF_S = 1024
TOP_K = 2
TOK_DEV = 128
TOKENS = 4096
EXPERTS = 32
CAP = 16
N_SP = 32
N_TP = 16


def draw_doc_ids(key, part):
    documents = max(2, N_SP // 4)
    spacing = TOKENS // documents
    offsets = jax.random.randint(jax.random.fold_in(key, 31), (documents - 1,), TOK_DEV // 4, 3 * TOK_DEV // 4 + 1)
    starts = jnp.arange(1, documents, dtype=jnp.int32) * spacing + offsets.astype(jnp.int32)
    positions = jnp.arange(TOKENS, dtype=jnp.int32)
    return jnp.sum((positions[:, None] >= starts[None, :]).astype(jnp.int32), axis=1).astype(jnp.int32)


def draw_pool_input(key, part):
    noise_key, level_key = jax.random.split(jax.random.fold_in(key, 11))
    levels = jax.random.normal(level_key, (TOKENS // 16, PW), jnp.float32)
    levels = jnp.repeat(levels, 16, axis=0)
    noise = jax.random.normal(noise_key, (TOKENS, PW), jnp.float32)
    values = noise + 1.5 * levels
    return jnp.clip(values, -12.0, 12.0).astype(jnp.bfloat16)


def draw_residual(key, part):
    noise_key, column_key = jax.random.split(jax.random.fold_in(key, 23))
    position = jnp.arange(D, dtype=jnp.float32) / (D - 1)
    noise = jax.random.normal(noise_key, (TOKENS, D), jnp.float32)
    scales = jnp.exp(jnp.log(3.0) * position + jax.random.uniform(column_key, (D,), jnp.float32, -0.5, 0.5))
    return jnp.clip(noise * scales[None, :], -30.0, 30.0).astype(jnp.bfloat16)


def strengthened(array, rng, source, target, shards_of, factor):
    def block_of(dim):
        return (jnp.arange(array.shape[dim]) // (array.shape[dim] // shards_of)).reshape((-1,) + (1,) * (array.ndim - 1 - dim))

    one_side = jax.random.permutation(rng, shards_of)[block_of(target)]
    far = (block_of(target) + shards_of // 2) % shards_of
    return jnp.where((block_of(source) == one_side) | (block_of(source) == far), factor * array, array)


def block_scale(rng, extent, cuts, least, high):
    level = 1.0
    for dim, parts in cuts:
        draws = jax.random.uniform(jax.random.fold_in(jax.random.fold_in(rng, 6), dim), (parts,), jnp.float32, least / len(cuts), high / len(cuts))
        level = level * jnp.repeat(jnp.exp(draws), extent[dim] // parts).reshape((-1,) + (1,) * (len(extent) - 1 - dim))
    return level


def assign_block(rng, own, number, rows, number_of, top, reach, skew):
    ranking = jax.random.permutation(rng, number_of)
    crowded, usual = portions_of(number_of, rows * top, reach, skew, True), portions_of(number_of, rows * top, reach, skew, False)
    places = jnp.arange(number_of)

    def named(lengths, turn):
        used = int((lengths > 0).sum())
        fixed = max(1, used // 4)
        passed = fixed + (places - fixed + turn * (used - fixed)) % max(1, number_of - fixed)
        return jnp.zeros((number_of,), jnp.int32).at[ranking[jnp.where(places < fixed, places, passed)]].set(jnp.asarray(lengths, jnp.int32))

    lengths = jnp.where(number % 4 == 0, named(crowded, number // 4), named(usual, number - number // 4 - 1))
    mixed = jax.random.permutation(jax.random.fold_in(own, 3), number_of)
    source_of, receiver = mixed[0:number_of // 2 * 2:2], mixed[1:number_of // 2 * 2:2]
    room = jnp.minimum(lengths[source_of] - 1, reach - lengths[receiver]) // 2
    room = jnp.where((source_of == ranking[0]) | (receiver == ranking[0]) | (lengths[receiver] == 0), 0, jnp.maximum(room, 0))
    passed = jax.random.randint(jax.random.fold_in(own, 4), (number_of // 2,), 0, 1 << 20) % (room + 1)
    lengths = lengths.at[source_of].add(-passed).at[receiver].add(passed)
    labels = jnp.searchsorted(jnp.cumsum(lengths), jnp.arange(rows * top), side="right").astype(jnp.int32)
    grid = labels.reshape(top, rows).T
    grid = grid[jax.random.permutation(jax.random.fold_in(own, 1), rows)]
    turn = jax.random.randint(jax.random.fold_in(own, 2), (rows, 1), 0, top)
    return jnp.take_along_axis(grid, (jnp.arange(top)[None, :] + turn) % top, axis=1)


def portions_of(count, total, limit, slope, full):
    loads = [(1 << 20) // math.isqrt(rank ** slope) + 1 for rank in range(1, count + 1)]
    largest = limit if full else min(limit, max(-(-total // count), total * loads[0] // sum(loads)))
    least = 1 if total - largest >= count - 1 else 0
    holding, spare = [largest] + [least] * (count - 1), total - largest - least * (count - 1)
    while spare > 0:
        movable = [i for i in range(1, count) if holding[i] < largest] or [i for i in range(1, count) if holding[i] < limit]
        mass, left = sum([loads[i] for i in movable]), spare
        for i in movable:
            extra = min(limit - holding[i], max(1, left * loads[i] // mass), spare)
            holding[i] = holding[i] + extra
            spare = spare - extra
    return np.array(holding)


def centred(key, dims, spread, limit, cuts=(), kind=jnp.bfloat16):
    drawn = jax.random.normal(key, dims, jnp.float32) * spread
    if len(cuts) > 0:
        drawn = block_scale(key, dims, cuts, -0.22, 0.18) * drawn
    return jnp.clip(drawn, min=-limit, max=limit).astype(kind)


def bell_draw_with(key, extent, spread, most, cuts, heavy, kind=jnp.bfloat16):
    values = spread * jax.random.normal(key, extent, jnp.float32)
    if cuts:
        values = values * block_scale(key, extent, cuts, -0.22, 0.18)
    return jnp.clip(strengthened(values, jax.random.fold_in(key, 3), *heavy), -most, most).astype(kind)


def setup_inputs(seed: int = 0) -> dict:
    arg_keys = jax.random.split(jax.random.key(seed), 15)
    pool_input = draw_pool_input(jax.random.fold_in(arg_keys[14], 71), 0)
    doc_ids = draw_doc_ids(jax.random.fold_in(arg_keys[14], 71), 0)
    residual = draw_residual(jax.random.fold_in(arg_keys[14], 71), 0)
    pool_gain = jnp.clip(1.0 + 0.18 * jax.random.normal(arg_keys[3], (PW,), jnp.float32), 0.1, 1.9)
    out_proj = bell_draw_with(arg_keys[4], (PW, D), PW ** -0.5, 0.25, ((0, 16),), (0, 1, 16, 2.0))
    norm_gain = jnp.clip(1.0 + 0.18 * jax.random.normal(arg_keys[5], (D,), jnp.float32), 0.1, 1.9)
    routes_keys = jax.random.split(jax.random.fold_in(arg_keys[6], 1), TOKENS // TOK_DEV)
    routes_turns = jax.random.permutation(jax.random.fold_in(arg_keys[6], 3), TOKENS // TOK_DEV)
    routes = jax.vmap(lambda own, number: assign_block(jax.random.fold_in(arg_keys[6], 2), own, number, TOK_DEV, EXPERTS, TOP_K, CAP, 1))(routes_keys, routes_turns).reshape((TOKENS, TOP_K))
    route_weights = jnp.clip(jnp.exp(math.log(1.2) - 1.7917595 * jax.random.uniform(arg_keys[7], (TOKENS, TOP_K), jnp.float32) ** block_scale(arg_keys[7], (TOKENS, TOP_K), ((0, 32),), -0.2, 0.2)), 0.2, 1.2)
    expert_gate = centred(arg_keys[8], (EXPERTS, D, FF_E), D ** -0.5, 0.125, ((0, 32), (2, 16)))
    expert_up = centred(arg_keys[9], (EXPERTS, D, FF_E), D ** -0.5, 0.125, ((0, 32), (2, 16)))
    expert_down = bell_draw_with(arg_keys[10], (EXPERTS, FF_E, D), FF_E ** -0.5, 0.125, ((0, 32), (1, 16)), (1, 2, 16, 2.0))
    shared_gate = centred(arg_keys[11], (D, FF_S), D ** -0.5, 0.125, ((1, 16),))
    shared_up = centred(arg_keys[12], (D, FF_S), D ** -0.5, 0.125, ((1, 16),))
    shared_down = bell_draw_with(arg_keys[13], (FF_S, D), FF_S ** -0.5, 0.25, ((0, 16),), (0, 1, 16, 2.0))
    return {"pool_input": pool_input, "doc_ids": doc_ids, "residual": residual, "pool_gain": pool_gain, "out_proj": out_proj, "norm_gain": norm_gain, "routes": routes, "route_weights": route_weights, "expert_gate": expert_gate, "expert_up": expert_up, "expert_down": expert_down, "shared_gate": shared_gate, "shared_up": shared_up, "shared_down": shared_down}


def blocked_down(hidden, down_weight, groups):
    width = hidden.shape[1] // groups
    pieces = jnp.moveaxis(hidden.reshape(hidden.shape[0], groups, width), 1, 0)
    weights = down_weight.reshape(groups, width, down_weight.shape[1])

    def add_group(accumulated, pair):
        product = jnp.dot(pair[0], pair[1], preferred_element_type=jnp.float32)
        rounded = lax.optimization_barrier(product.astype(jnp.bfloat16))
        return (accumulated + rounded.astype(jnp.float32), None)
    initial = jnp.zeros((hidden.shape[0], down_weight.shape[1]), jnp.float32)
    summed, unused = lax.scan(add_group, initial, (pieces, weights))
    return summed.astype(jnp.bfloat16)

def reference(pool_input, doc_ids, residual, pool_gain, out_proj, norm_gain, routes, route_weights, expert_gate, expert_up, expert_down, shared_gate, shared_up, shared_down):
    values = pool_input.astype(jnp.float32)
    positions = jnp.arange(TOKENS, dtype=jnp.int32)
    begins = jnp.concatenate([jnp.ones((1,), bool), doc_ids[1:] != doc_ids[:-1]])
    doc_start = lax.cummax(jnp.where(begins, positions, 0), axis=0)
    length = (positions - doc_start + 1).astype(jnp.float32)
    scale_index = jnp.arange(PW, dtype=jnp.int32) % 4
    window_size = jnp.where(scale_index == 0, 2.0, jnp.where(scale_index == 1, 8.0, 16.0))
    padded = jnp.concatenate([jnp.zeros((15, PW), jnp.float32), values], 0)
    window_total = jnp.zeros((TOKENS, PW), jnp.float32)
    for offset in range(16):
        inside = (offset < length[:, None]) & (offset < window_size[None, :])
        window_total = window_total + jnp.where(inside, padded[15 - offset:15 - offset + TOKENS], 0.0)
    window_mean = window_total / jnp.minimum(length[:, None], window_size[None, :])
    running = jnp.cumsum(values[:, 3::4], axis=0)
    shifted = jnp.concatenate([jnp.zeros((1, PW // 4), jnp.float32), running], 0)
    doc_sum = running - jnp.take(shifted, doc_start, axis=0)
    doc_mean = doc_sum / length[:, None]
    pool_mean = jnp.concatenate([window_mean.reshape(TOKENS, PW // 4, 4)[..., :3], doc_mean[..., None]], -1)
    pool_mean = pool_mean.reshape(TOKENS, PW)
    pooled = ((pool_mean - values) * pool_gain).astype(jnp.bfloat16)
    projected = blocked_down(pooled, out_proj, N_TP)
    hidden_state = residual.astype(jnp.float32) + projected.astype(jnp.float32)
    squares = lax.optimization_barrier(jnp.mean(hidden_state * hidden_state, axis=1, keepdims=True))
    normed = (hidden_state * lax.rsqrt(squares + 1e-06) * norm_gain).astype(jnp.bfloat16)
    flat_experts = routes.reshape(N_SP, TOK_DEV * TOP_K)
    onehot = (flat_experts[..., None] == jnp.arange(EXPERTS, dtype=jnp.int32)).astype(jnp.int32)
    ranks = lax.optimization_barrier(jnp.sum((jnp.cumsum(onehot, axis=1) - 1) * onehot, axis=2))
    block_ids = jnp.arange(N_SP, dtype=jnp.int32)[:, None]
    slot_index = ((flat_experts * N_SP + block_ids) * CAP + ranks).reshape(-1).astype(jnp.int32)
    token_index = (jnp.arange(TOKENS * TOP_K, dtype=jnp.int32) // TOP_K).astype(jnp.int32)
    table_rows = EXPERTS * N_SP * CAP
    slot_token = jnp.full((table_rows,), TOKENS, jnp.int32).at[slot_index].set(token_index)
    with_blank = jnp.concatenate([normed, jnp.zeros((1, D), jnp.bfloat16)], 0)
    expert_rows = jnp.take(with_blank, slot_token, axis=0).reshape(EXPERTS, N_SP * CAP, D)

    def run_expert(group):
        rows_in, gate_weight, up_weight, down_weight = group
        gate = jnp.dot(rows_in, gate_weight, preferred_element_type=jnp.float32)
        upper = jnp.dot(rows_in, up_weight, preferred_element_type=jnp.float32)
        hidden = (jax.nn.silu(gate) * upper).astype(jnp.bfloat16)
        return blocked_down(hidden, down_weight, N_TP)
    expert_out = lax.map(run_expert, (expert_rows, expert_gate, expert_up, expert_down)).reshape(table_rows, D)
    picked = jnp.take(expert_out, slot_index, axis=0).astype(jnp.float32) * route_weights.reshape(-1)[:, None]
    routed = lax.optimization_barrier(jnp.sum(picked.reshape(TOKENS, TOP_K, D), axis=1))
    shared_gate_out = jnp.dot(normed, shared_gate, preferred_element_type=jnp.float32)
    shared_up_out = jnp.dot(normed, shared_up, preferred_element_type=jnp.float32)
    shared_hidden = (jax.nn.silu(shared_gate_out) * shared_up_out).astype(jnp.bfloat16)
    shared_out = blocked_down(shared_hidden, shared_down, N_TP)
    return (hidden_state + routed + shared_out.astype(jnp.float32)).astype(jnp.bfloat16)
```

```python
import functools

import jax
import jax.numpy as jnp
from jax import lax
from jax.experimental import pallas as pl
from jax.experimental.pallas import tpu as pltpu
from jax.sharding import PartitionSpec as P

MESH = pl.DeviceIdType.MESH
F32 = jnp.float32
BF16 = jnp.bfloat16
VMEM = pltpu.VMEM
DMA = pltpu.SemaphoreType.DMA


def dot(a, b):
    return jnp.dot(a, b, preferred_element_type=F32)


def dot_nt(a, b):
    return lax.dot_general(a, b, (((1,), (1,)), ((), ())), preferred_element_type=F32)


def dot_tn(a, b):
    return lax.dot_general(a, b, (((0,), (0,)), ((), ())), preferred_element_type=F32)


def silu(v):
    return v * (1.0 / (1.0 + jnp.exp(-v)))


def iota(shape, dim):
    return lax.broadcasted_iota(jnp.int32, shape, dim)


def ones_where(mask):
    return jnp.where(mask, 1.0, 0.0)


def as_columns(row, size):
    return jnp.transpose(jnp.broadcast_to(row, (size, size)))


def kernel(
    cfg,
    xt_ref, ids_ref, residual_ref, pgain_ref, ngain_ref, routes_ref, weights_ref,
    oproj_hbm, eg_hbm, eu_hbm, ed_hbm, sg_hbm, su_hbm, sd_hbm,
    out_ref,
    oproj, eg, eu, ed, sgu, sd, local_sem,
    cb, xprev, wq, gn, pk, dsp, big, part, qbuf, ra, rb, sa, sb, fin, back,
    gbuf, hbuf, accg, accu, ssq, accs, sss, slot_scr,
    send, carry_sem, rim_sem, wq_sem, gn_sem, pk_sem, disp_sem, ring_a, ring_b,
    peer_sem, q_sem, rs_a, rs_b, back_sem,
):
    NS, NT, T, CAP, NCH = cfg
    Y = NT // 2
    R = NS * CAP
    RC = R // NCH
    BPC = NS // NCH
    NA, NB = Y // 2, Y - 1 - Y // 2
    D = NT * T
    s = lax.axis_index("sp")
    me = lax.axis_index("tp")
    y = me // 2
    c = me % 2
    partner = (s, y * 2 + 1 - c)
    sign = 1 - 2 * c

    def chip(off):
        return lax.rem(y + off + 2 * Y, Y)

    def rcopy(src, dst, ssem, rsem, dev):
        return pltpu.make_async_remote_copy(
            src_ref=src, dst_ref=dst, send_sem=ssem, recv_sem=rsem, device_id=dev, device_id_type=MESH
        )

    def arrived(ref, rsem):
        rcopy(ref, ref, send.at[0], rsem, partner).wait_recv()

    def sent(ref, k):
        rcopy(ref, ref, send.at[k], rim_sem.at[0], partner).wait_send()

    loads = [
        pltpu.make_async_copy(src, dst, local_sem.at[k])
        for k, (src, dst) in enumerate(
            [
                (oproj_hbm, oproj),
                (eg_hbm.at[0], eg),
                (eu_hbm.at[0], eu),
                (ed_hbm.at[0], ed),
                (sg_hbm, sgu.at[pl.ds(0, 64)]),
                (su_hbm, sgu.at[pl.ds(64, 64)]),
                (sd_hbm, sd),
            ]
        )
    ]
    for load in loads:
        load.start()

    barrier = pltpu.get_barrier_semaphore()

    def greet_sp(k, _):
        pl.semaphore_signal(barrier, inc=1, device_id=(lax.rem(s + k, NS), me), device_id_type=MESH)
        return 0

    def greet_tp(k, _):
        pl.semaphore_signal(barrier, inc=1, device_id=(s, lax.rem(me + k, NT)), device_id_type=MESH)
        return 0

    lax.fori_loop(1, NS, greet_sp, 0)
    lax.fori_loop(1, NT, greet_tp, 0)

    xt = xt_ref[...]
    ids = ids_ref[...].astype(F32)
    lane1 = iota((1, T), 1)
    d0 = jnp.sum(jnp.where(lane1 == 0, ids, 0.0), axis=1, keepdims=True)
    d_last = jnp.sum(jnp.where(lane1 == T - 1, ids, 0.0), axis=1, keepdims=True)
    tail = ones_where(ids == d_last)
    tail_len = jnp.sum(tail, axis=1, keepdims=True)
    tail_sum = dot_nt(jnp.broadcast_to(tail, (8, T)).astype(BF16), xt)[0:1, :]
    cb[pl.ds(s, 1), :, :] = jnp.where(
        lane1 == 0, tail_len, jnp.where(lane1 == 1, d_last, 0.0)
    ).reshape(1, 1, T)
    cb[pl.ds(s, 1), :, 64:128] = tail_sum.reshape(1, 1, 64)
    gn[pl.ds(me, 1), :, :] = ngain_ref[...].reshape(1, 1, T)

    loads[0].wait()
    pl.semaphore_wait(barrier, NS - 1 + NT - 1)

    def send_carry(k, _):
        to = (lax.rem(s + k, NS), me)
        rcopy(cb.at[s], cb.at[s], send.at[0], carry_sem.at[0], to).start()
        return 0

    lax.fori_loop(1, NS, send_carry, 0)
    rcopy(xt_ref, xprev, send.at[3], rim_sem.at[0], (lax.rem(s + 1, NS), me)).start()

    def send_proj(k, _):
        j = lax.rem(me + k, NT)
        to = (s, j)
        cols = oproj.at[:, pl.ds(pl.multiple_of(j * T, T), T)]
        rcopy(cols, wq.at[me], send.at[1], wq_sem.at[0], to).start()
        rcopy(gn.at[me], gn.at[me], send.at[2], gn_sem.at[0], to).start()
        return 0

    lax.fori_loop(1, NT, send_proj, 0)
    wq[pl.ds(me, 1), :, :] = oproj[:, pl.ds(pl.multiple_of(me * T, T), T)].reshape(1, 64, T)

    su_i, la_i = iota((T, T), 0), iota((T, T), 1)
    ids_t = jnp.broadcast_to(ids, (T, T))
    causal = (jnp.transpose(ids_t) == ids_t) & (su_i <= la_i)
    windows = (2, 8, 16)
    scale = lax.rem(iota((64, T), 0), 4)

    def by_scale(a0, a1, a2, a3):
        return jnp.where(scale == 0, a0, jnp.where(scale == 1, a1, jnp.where(scale == 2, a2, a3)))

    own = [dot(xt, ones_where(causal & (la_i - su_i < w)).astype(BF16)) for w in windows]
    all_own = ones_where(causal)
    total = by_scale(*own, dot(xt, all_own.astype(BF16)))
    count = jnp.sum(all_own, axis=0, keepdims=True)
    gbuf[...] = jnp.zeros_like(gbuf)
    gbuf[:, 0:64] = pgain_ref[...]
    gain_t = as_columns(gbuf[...], T)[0:64, :]

    experts = routes_ref[...]
    hits = [ones_where(iota((T, T), 0) == experts[k : k + 1, :]) for k in range(2)]
    earlier = dot((hits[0] + hits[1]).astype(BF16), ones_where(su_i < la_i).astype(BF16))
    slots = [
        experts[k : k + 1, :].astype(F32) * CAP
        + jnp.sum(earlier * hits[k], axis=0, keepdims=True)
        for k in range(2)
    ]
    for k in range(2):
        slot_scr[k : k + 1, :] = slots[k]

    arrived(cb.at[pl.ds(0, NS - 1)], carry_sem.at[0])
    tails = cb[...]
    lane3 = iota((NS, 1, T), 2)
    last_ids = jnp.sum(jnp.where(lane3 == 1, tails, 0.0), axis=2, keepdims=True)
    used = (iota((NS, 1, T), 0) < s) & (last_ids == d0.reshape(1, 1, 1))
    carried = jnp.sum(jnp.where(used, tails, 0.0), axis=0)
    carry_len = jnp.sum(jnp.where(lane1 == 0, carried, 0.0), axis=1, keepdims=True)
    carry_t = as_columns(carried, T)[64:128, :]
    first_doc = ids == d0
    length = count + jnp.where(first_doc, carry_len, 0.0)
    arrived(xprev, rim_sem.at[0])
    before = (su_i.astype(F32) >= T - carry_len) & first_doc
    prev = xprev[...]
    past = [dot(prev, ones_where(before & (la_i + T - su_i < w)).astype(BF16)) for w in windows]
    total = total + by_scale(*past, jnp.where(first_doc, carry_t, 0.0))
    spans = [jnp.broadcast_to(jnp.minimum(length, float(w)), (64, T)) for w in windows]
    mean = total / by_scale(*spans, jnp.broadcast_to(length, (64, T)))
    pooled = ((mean - xt.astype(F32)) * gain_t).astype(BF16)
    pk[pl.ds(me, 1), :, :] = pooled.reshape(1, 64, T)

    def give_partner(j):
        rcopy(pk.at[j], pk.at[j], send.at[4], pk_sem.at[j], partner).start()

    far_first = sorted([o for o in range(1, Y)], key=lambda o: -min(o, Y - o))
    for off in far_first:
        to = (s, chip(off) * 2 + c)
        rcopy(pk.at[me], pk.at[me], send.at[4], pk_sem.at[me], to).start()
    give_partner(me)
    for off in reversed(far_first):
        j = chip(off) * 2 + c
        arrived(pk.at[j], pk_sem.at[j])
        give_partner(j)
    arrived(wq.at[pl.ds(0, NT - 1)], wq_sem.at[0])
    for off in [0] + list(reversed(far_first)):
        j = chip(off) * 2 + 1 - c
        arrived(pk.at[j], pk_sem.at[j])
    projected = dot_tn(pk[...].reshape(NT * 64, T), wq[...].reshape(NT * 64, T)).astype(BF16)
    hidden_state = residual_ref[...].astype(F32) + projected.astype(F32)
    hbuf[...] = hidden_state
    rows = hidden_state.astype(BF16)
    big[pl.ds(me, 1), 0:T, :] = rows.reshape(1, T, T)

    srow = iota((R, T), 0).astype(F32)
    chosen = ones_where((srow == slot_scr[0:1, :]) | (srow == slot_scr[1:2, :])).astype(BF16)
    dsp[...] = dot(chosen, rows).astype(BF16)

    def block_rows(ref, b, base=0):
        return ref.at[pl.ds(pl.multiple_of(base + b * CAP, 16), CAP)]

    def send_rows(k, _):
        b = lax.rem(s + k, NS)
        rcopy(
            block_rows(dsp, b), block_rows(big.at[me], s, T), send.at[5], disp_sem.at[s], (b, me)
        ).start()
        return 0

    lax.fori_loop(1, NS, send_rows, 0)
    big[pl.ds(me, 1), pl.ds(pl.multiple_of(T + s * CAP, 16), CAP), :] = dsp[
        pl.ds(pl.multiple_of(s * CAP, 16), CAP), :
    ].reshape(1, CAP, T)

    def span(i):
        return pl.ds(0, T) if i == 0 else pl.ds(T + (i - 1) * RC, RC)

    flows = ((NA, sign, ring_a), (NB, -sign, ring_b))
    CH = NCH + 1

    def to_peer(j, i):
        ref = big.at[j, span(i)]
        rcopy(ref, ref, send.at[6], peer_sem.at[j // 2, i], partner).start()

    def to_ring(flow, j, k, i):
        n, sg, sems = flows[flow]
        ref = big.at[j, span(i)]
        rcopy(ref, ref, send.at[6], sems.at[k, i], (s, chip(sg) * 2 + c)).start()

    def begin(i):
        to_ring(0, me, 0, i)
        to_ring(1, me, 0, i)
        to_peer(me, i)

    def hop(k, i):
        for flow in (0, 1):
            n, sg, sems = flows[flow]
            if k <= n:
                j = chip(-sg * k) * 2 + c
                arrived(big.at[j, span(i)], sems.at[k - 1, i])
                if k < n:
                    to_ring(flow, j, k, i)
                to_peer(j, i)

    def take(ref, o, part_rows):
        a = ref[pl.ds(2 * o, 1), part_rows, :].reshape(-1, T).astype(F32)
        b = ref[pl.ds(2 * o + 1, 1), part_rows, :].reshape(-1, T).astype(F32)
        ga = gn[pl.ds(2 * o, 1), :, :].reshape(1, T)
        gb = gn[pl.ds(2 * o + 1, 1), :, :].reshape(1, T)
        both = jnp.concatenate([(a * ga).astype(BF16), (b * gb).astype(BF16)], axis=1)
        return both, a * a + b * b

    def cols(o):
        return pl.ds(pl.multiple_of(o * 2 * T, 2 * T), 2 * T)

    def add_to(ref, value, first):
        ref[...] = value if first else ref[...] + value

    def routed_in(o, first=False):
        for i in range(1, CH):
            ref = big.at[2 * o + 1 - c, span(i)]
            arrived(ref, peer_sem.at[o, i])
        both, squares = take(big, o, slice(T, T + R))
        add_to(ssq, squares, first)
        add_to(accg, dot(both, eg[cols(o), :]), first)
        add_to(accu, dot(both, eu[cols(o), :]), first)

    def shared_in(o, first=False):
        arrived(big.at[2 * o + 1 - c, span(0)], peer_sem.at[o, 0])
        both, squares = take(big, o, slice(0, T))
        add_to(sss, squares, first)
        add_to(accs, dot_nt(both, sgu[:, cols(o)]), first)

    begin(0)
    early = min(2, NA)
    for k in range(1, early + 1):
        hop(k, 0)
    arrived(gn.at[pl.ds(0, NT - 1)], gn_sem.at[0])
    for i in range(1, CH):

        def wait_rows(q, _, i=i):
            b = (i - 1) * BPC + q

            @pl.when(b != s)
            def _():
                arrived(block_rows(big.at[me], b, T), disp_sem.at[b])

            return 0

        lax.fori_loop(0, BPC, wait_rows, 0)
        begin(i)
    for k in range(early + 1, NA + 1):
        hop(k, 0)
    for load in loads[1:]:
        load.wait()
    shared_in(y, True)
    for off in range(1, Y):
        shared_in(chip(off))
    model_scale = 1.0 / D
    rs_s = lax.rsqrt(jnp.sum(sss[...], axis=1, keepdims=True) * model_scale + 1e-6)
    sh = accs[...] * rs_s
    sh_hidden = (silu(sh) * pltpu.roll(sh, 64, 1))[:, 0:64].astype(BF16)
    for k in range(1, NA + 1):
        for i in range(1, CH):
            hop(k, i)
        if k == 1:
            routed_in(y, True)
        else:
            routed_in(chip(k - 1))
            routed_in(chip(1 - k))
    if NB == NA - 1:
        routed_in(chip(NA))
    rs_r = lax.rsqrt(jnp.sum(ssq[...], axis=1, keepdims=True) * model_scale + 1e-6)
    hidden = (silu(accg[...] * rs_r) * (accu[...] * rs_r)).astype(BF16)

    def down(o):
        v = dot(hidden, ed[:, cols(o)]).astype(BF16)
        part[pl.ds(2 * o, 1), T : T + R, :] = v[:, 0:T].reshape(1, R, T)
        part[pl.ds(2 * o + 1, 1), T : T + R, :] = v[:, T : 2 * T].reshape(1, R, T)
        give(o, pl.ds(T, R), 0)

    def shared_down(o):
        v = dot(sh_hidden, sd[:, cols(o)]).astype(BF16)
        part[pl.ds(2 * o, 1), 0:T, :] = v[:, 0:T].reshape(1, T, T)
        part[pl.ds(2 * o + 1, 1), 0:T, :] = v[:, T : 2 * T].reshape(1, T, T)
        give(o, pl.ds(0, T), 1)

    def give(o, where, k):
        rcopy(
            part.at[2 * o + 1 - c, where], qbuf.at[o, where], send.at[7], q_sem.at[o, k], partner
        ).start()

    def pair_sum(o, i):
        where = span(i)
        if i == 0:
            arrived(qbuf.at[o, pl.ds(0, T)], q_sem.at[o, 1])
        elif i == 1:
            arrived(qbuf.at[o, pl.ds(T, R)], q_sem.at[o, 0])
        mine = part[pl.ds(2 * o + c, 1), where, :].astype(F32)
        return mine[0] + qbuf[pl.ds(o, 1), where, :].astype(F32)[0]

    rings = ((NA, sign, rs_a, ra, sa), (NB, -sign, rs_b, rb, sb))

    def rs_step(flow, j, i):
        n, sg, sems, got, out = rings[flow]
        if j > n:
            return
        where = span(i)
        value = pair_sum(chip(sg * (n - j + 1)), i)
        if j > 1:
            arrived(got.at[j - 2, where], sems.at[j - 2, i])
            value = value + got[j - 2, where, :].astype(F32)
        out[j - 1, where, :] = value.astype(BF16)
        rcopy(
            out.at[j - 1, where], got.at[j - 1, where], send.at[8], sems.at[j - 1, i],
            (s, chip(sg) * 2 + c),
        ).start()

    def rs_end(i):
        where = span(i)
        value = pair_sum(y, i)
        for n, sg, sems, got, out in rings:
            arrived(got.at[n - 1, where], sems.at[n - 1, i])
            value = value + got[n - 1, where, :].astype(F32)
        fin[where, :] = value.astype(BF16)

    def send_back(q, _):
        @pl.when(q != s)
        def _():
            rcopy(
                block_rows(fin, q, T), block_rows(back, s), send.at[9], back_sem.at[0], (q, me)
            ).start()

        return 0

    order = sorted(range(Y), key=lambda o: -min(o, Y - o))
    for off in order[:3]:
        down(chip(off))
    for i in range(1, CH):
        rs_step(0, 1, i)
        rs_step(1, 1, i)
    for off in order[3:]:
        down(chip(off))
    for o in range(Y):
        shared_down(chip(o))
    for j in range(2, NA + 1):
        for i in range(1, CH):
            rs_step(0, j, i)
            rs_step(1, j, i)
    rs_step(0, 1, 0)
    rs_step(1, 1, 0)
    for i in range(1, CH):
        rs_end(i)
        lax.fori_loop((i - 1) * BPC, i * BPC, send_back, 0)
    back[pl.ds(pl.multiple_of(s * CAP, 16), CAP), :] = fin[
        pl.ds(pl.multiple_of(T + s * CAP, 16), CAP), :
    ]
    for j in range(2, NA + 1):
        rs_step(0, j, 0)
        rs_step(1, j, 0)
    rs_end(0)

    arrived(back.at[pl.ds(0, R - CAP)], back_sem.at[0])
    result = hbuf[...] + fin[0:T, :].astype(F32)
    for k in range(2):
        slot_cols = as_columns(slot_scr[k : k + 1, :], T)
        picks = jnp.concatenate(
            [
                ones_where(slot_cols == (la_i + q * T).astype(F32)).astype(BF16)
                for q in range(R // T)
            ],
            axis=1,
        )
        result = result + as_columns(weights_ref[k : k + 1, :], T) * dot(picks, back[...])
    out_ref[...] = result.astype(BF16)

    sent(cb.at[pl.ds(0, NS - 1)], 0)
    sent(wq.at[pl.ds(0, NT - 1)], 1)
    sent(gn.at[pl.ds(0, NT - 1)], 2)
    sent(xprev, 3)
    sent(pk.at[pl.ds(0, NT - 1)], 4)
    sent(dsp.at[pl.ds(0, R - CAP)], 5)
    sent(big.at[pl.ds(0, NT - 1)], 6)
    sent(qbuf, 7)
    sent(qbuf.at[pl.ds(0, Y - 1)], 8)
    sent(back.at[pl.ds(0, R - CAP)], 9)


def layer(cfg, *args):
    (pool_input, doc_ids, residual, pool_gain, out_proj, norm_gain, routes, route_weights,
     expert_gate, expert_up, expert_down, shared_gate, shared_up, shared_down) = args
    NS, NT, T, CAP, NCH = cfg
    Y = NT // 2
    R = NS * CAP
    NA, NB = Y // 2, Y - 1 - Y // 2
    CH = NCH + 1
    D = NT * T
    E = T + R
    FH = expert_gate.shape[2]
    inputs = (
        pool_input.T, doc_ids.reshape(1, T), residual, pool_gain.reshape(1, -1),
        norm_gain.reshape(1, T), routes.T, route_weights.T,
        out_proj, expert_gate, expert_up, expert_down, shared_gate.T, shared_up.T, shared_down,
    )
    vm = pl.BlockSpec(memory_space=pltpu.VMEM)
    hbm = pl.BlockSpec(memory_space=pl.ANY)
    scratch = [
        VMEM((64, D), BF16), VMEM((D, FH), BF16), VMEM((D, FH), BF16), VMEM((FH, D), BF16),
        VMEM((128, D), BF16), VMEM((64, D), BF16), DMA((7,)),
        VMEM((NS, 1, T), F32), VMEM((64, T), BF16), VMEM((NT, 64, T), BF16),
        VMEM((NT, 1, T), F32), VMEM((NT, 64, T), BF16), VMEM((R, T), BF16),
        VMEM((NT, E, T), BF16), VMEM((NT, E, T), BF16), VMEM((Y, E, T), BF16),
        VMEM((NA, E, T), BF16), VMEM((NB, E, T), BF16), VMEM((NA, E, T), BF16),
        VMEM((NB, E, T), BF16), VMEM((E, T), BF16), VMEM((R, T), BF16),
        VMEM((1, T), F32), VMEM((T, T), F32), VMEM((R, FH), F32), VMEM((R, FH), F32),
        VMEM((R, T), F32), VMEM((T, 128), F32), VMEM((T, T), F32), VMEM((8, T), F32),
        DMA((10,)), DMA((1,)), DMA((1,)), DMA((1,)), DMA((1,)), DMA((NT,)), DMA((NS,)),
        DMA((NA, CH)), DMA((NB, CH)), DMA((Y, CH)), DMA((Y, 2)), DMA((NA, CH)), DMA((NB, CH)),
        DMA((1,)),
    ]
    return pl.pallas_call(
        functools.partial(kernel, cfg),
        out_shape=jax.ShapeDtypeStruct((T, T), BF16),
        in_specs=[vm] * 7 + [hbm] * 7,
        out_specs=vm,
        scratch_shapes=scratch,
        compiler_params=pltpu.CompilerParams(
            collective_id=0, has_side_effects=True, vmem_limit_bytes=67043328
        ),
    )(*inputs)


def solution(mesh, cap=None):
    NS, NT = mesh.shape["sp"], mesh.shape["tp"]
    placed = (
        P("sp", "tp"), P("sp"), P("sp", "tp"), P("tp"), P("tp", None), P("tp"), P("sp", None),
        P("sp", None), P("sp", None, "tp"), P("sp", None, "tp"), P("sp", "tp", None),
        P(None, "tp"), P(None, "tp"), P("tp", None),
    )

    def body(*args):
        T = args[1].shape[0]
        top = args[6].shape[1]
        most = cap or 16 * max(1, 2 * T * top // (NS * 16))
        return layer((NS, NT, T, most, min(4, NS)), *args)

    return jax.shard_map(body, mesh=mesh, in_specs=placed, out_specs=P("sp", "tp"), check_vma=False)
```
